128 devices in a mesh: sp: 16 (over z, y), tp: 8 (over x, core).
Axes of the slice: x: 4, y: 4, z: 4, core: 2. Of those that a mesh axis runs over, the one named last changes fastest.
Arguments:
- tokens: bfloat16 [6144, 4096], P(('sp', 'tp')), may hold values from -6 to 6
- norm_gain: bfloat16 [4096], replicated, may hold values from 0.099609375 to 1.8984375
- w_pool_in: bfloat16 [4096, 4096], P('sp', 'tp'), may hold values from -0.09375 to 0.09375
- w_mem_in: bfloat16 [4096, 4096], P('sp', 'tp'), may hold values from -0.09375 to 0.09375
- w_input_gate: bfloat16 [4096, 16], replicated, may hold values from -104 to 104
- w_forget_gate: bfloat16 [4096, 16], replicated, may hold values from -0.09375 to 0.09375
- forget_bias: float32 [16], replicated, may hold values from 3 to 13
- forget_extra: float32 [6144, 16], P('sp', 'tp'), may hold values from 0 to 1.5
- conv_weight: bfloat16 [4, 4096], replicated, may hold values from -3 to 3
- query_map: bfloat16 [1024, 4, 4], replicated, may hold values from -3 to 3
- key_map: bfloat16 [1024, 4, 4], replicated, may hold values from -3 to 3
- pool_map: bfloat16 [16, 256, 256], P('tp'), may hold values from -0.375 to 0.375
- pool_gain: bfloat16 [4096], replicated, may hold values from 0.099609375 to 1.8984375
- mem_gain: bfloat16 [4096], replicated, may hold values from 0.099609375 to 1.8984375
- w_out_pool: bfloat16 [4096, 4096], P('tp', 'sp'), may hold values from -0.0625 to 0.0625
- w_out_mem: bfloat16 [4096, 4096], P('tp', 'sp'), may hold values from -0.0625 to 0.0625
Outputs:
- layer_out: bfloat16 [6144, 4096], P(('sp', 'tp'))
The draws below stay inside these ranges and needn't reach their ends.
All inputs are finite; a program needn't handle non-finite values.
Results may differ from the reference program's by a relative error of at most 0.019.
The reference program's roundings to bfloat16 on the way count: a program that leaves them out, or rounds other values in their place, can miss the bound.
Values may be sent and summed in bfloat16 or wider, within the bound.
No kernel may reach another device: no remote copies, remote signals or barrier semaphores. Data moves between devices by JAX's collectives and lax.ppermute only.
A program may use at most 128 MiB of HBM per device.

```python
import jax
import jax.numpy as jnp
from jax import lax

D = 4096
POOL = 4096
MEM = 4096
HEAD = 256
CONV = 4
BLOCK = 128
TOK_DEV = 384
MEMORY_HEADS = 16
GROUPS = 16
SEQUENCE_TOKENS = 6144
N_TP = 8


def draw_w_input_gate(key, part):
    reach_value = 3.0
    values = jax.random.uniform(jax.random.fold_in(key, 301), (D, MEMORY_HEADS), jnp.float32, -reach_value, reach_value)
    return values.astype(jnp.bfloat16)


def draw_forget_bias(key, part):
    pick_key, fast_key, slow_key = jax.random.split(jax.random.fold_in(key, 302), 3)
    slow_share = 0.5
    slow_heads = jax.random.bernoulli(pick_key, slow_share, (MEMORY_HEADS,))
    fast_value = jax.random.uniform(fast_key, (MEMORY_HEADS,), jnp.float32, 3.0, 3.8)
    slow_value = jnp.log(SEQUENCE_TOKENS * 1.0) + jax.random.uniform(slow_key, (MEMORY_HEADS,), jnp.float32, 1.5, 2.5)
    return jnp.where(slow_heads, slow_value, fast_value).astype(jnp.float32)


def draw_forget_extra(key, part):
    frequency_key, spike_key, quantity_key = jax.random.split(jax.random.fold_in(key, 303), 3)
    segments = SEQUENCE_TOKENS // TOK_DEV
    decay_rate = jnp.exp(jax.random.uniform(frequency_key, (segments, 1, MEMORY_HEADS), jnp.float32, jnp.log(0.1), jnp.log(0.8))) / SEQUENCE_TOKENS
    constant_level = jnp.broadcast_to(decay_rate, (segments, TOK_DEV, MEMORY_HEADS)).reshape(SEQUENCE_TOKENS, MEMORY_HEADS)
    spike_rows = jax.random.randint(spike_key, (2, MEMORY_HEADS), 0, SEQUENCE_TOKENS)
    quantities = -jnp.log(1.0 - jax.random.uniform(quantity_key, (2, MEMORY_HEADS), jnp.float32, 0.2, 0.5))
    location_rows = jnp.arange(SEQUENCE_TOKENS)[:, None, None] == spike_rows[None]
    spikes = jnp.sum(jnp.where(location_rows, quantities[None], 0.0), axis=1)
    return (constant_level + spikes).astype(jnp.float32)


def levels(own_key, extent, cuts, least, high):
    level, own = 1.0, jax.random.fold_in(own_key, 6)
    for axis_at, blocks in cuts:
        steps = jnp.exp(jax.random.uniform(jax.random.fold_in(own, axis_at), (blocks,), jnp.float32, least / len(cuts), high / len(cuts)))
        level = level * jnp.repeat(steps, extent[axis_at] // blocks).reshape([-1 if axis == axis_at else 1 for axis in range(len(extent))])
    return level


def bell_draw(rng, dims, deviation, bound, cuts=(), held_as=jnp.bfloat16):
    values = deviation * jax.random.normal(rng, dims, jnp.float32)
    if cuts:
        values = values * levels(rng, dims, cuts, -0.22, 0.18)
    return jnp.clip(values, -bound, bound).astype(held_as)


def setup_inputs(seed: int = 0) -> dict:
    arg_keys = jax.random.split(jax.random.key(seed), 17)
    return {
        "tokens": bell_draw(arg_keys[0], (SEQUENCE_TOKENS, D), 1.0, 6.0, ((0, 128),)),
        "norm_gain": jnp.clip(1.0 + 0.18 * jax.random.normal(arg_keys[1], (D,), jnp.float32), 0.099609375, 1.8984375).astype(jnp.bfloat16),
        "w_pool_in": bell_draw(arg_keys[2], (D, POOL), D ** -0.5, 0.09375, ((0, 16), (1, 8))),
        "w_mem_in": bell_draw(arg_keys[3], (D, MEM), D ** -0.5, 0.09375, ((0, 16), (1, 8))),
        "w_input_gate": draw_w_input_gate(jax.random.fold_in(arg_keys[16], 71), 0),
        "w_forget_gate": bell_draw(arg_keys[5], (D, MEMORY_HEADS), D ** -0.5, 0.09375),
        "forget_bias": draw_forget_bias(jax.random.fold_in(arg_keys[16], 71), 0),
        "forget_extra": draw_forget_extra(jax.random.fold_in(arg_keys[16], 71), 0),
        "conv_weight": bell_draw(arg_keys[8], (CONV, MEM), CONV ** -0.5, 3.0),
        "query_map": bell_draw(arg_keys[9], (MEM // 4, 4, 4), 4 ** -0.5, 3.0),
        "key_map": bell_draw(arg_keys[10], (MEM // 4, 4, 4), 4 ** -0.5, 3.0),
        "pool_map": bell_draw(arg_keys[11], (GROUPS, HEAD, HEAD), HEAD ** -0.5, 0.375, ((0, 8),)),
        "pool_gain": jnp.clip(1.0 + 0.18 * jax.random.normal(arg_keys[12], (POOL,), jnp.float32), 0.099609375, 1.8984375).astype(jnp.bfloat16),
        "mem_gain": jnp.clip(1.0 + 0.18 * jax.random.normal(arg_keys[13], (MEM,), jnp.float32), 0.099609375, 1.8984375).astype(jnp.bfloat16),
        "w_out_pool": bell_draw(arg_keys[14], (POOL, D), (POOL + MEM) ** -0.5, 0.0625, ((0, 8), (1, 16))),
        "w_out_mem": bell_draw(arg_keys[15], (MEM, D), (POOL + MEM) ** -0.5, 0.0625, ((0, 8), (1, 16))),
    }


epsilon = 1e-06
windows_all = (2, 4, 8, 16)
highest = lax.Precision.HIGHEST

def rms_rows(rows, gain):
    values = rows.astype(jnp.float32)
    factor = lax.rsqrt(lax.optimization_barrier(jnp.mean(values * values, axis=-1, keepdims=True)) + epsilon)
    return (values * factor * gain.astype(jnp.float32)).astype(jnp.bfloat16)

def rounded(values):
    return lax.optimization_barrier(values.astype(jnp.bfloat16)).astype(jnp.float32)

def pool_branch(pool_in, pool_map, pool_gain):
    values = pool_in.astype(jnp.float32)
    position = jnp.arange(1, SEQUENCE_TOKENS + 1).astype(jnp.float32)[:, None]
    outputs = []
    for group_index in range(GROUPS):
        window = windows_all[group_index % 4]
        columns = values[:, group_index * HEAD:(group_index + 1) * HEAD]
        padded = jnp.pad(columns, ((window, 0), (0, 0)))
        window_total = padded[window:window + SEQUENCE_TOKENS]
        for offset in range(1, window):
            window_total = window_total + padded[window - offset:window - offset + SEQUENCE_TOKENS]
        counts = jnp.minimum(position, float(window))
        centred = (window_total / counts - columns).astype(jnp.bfloat16)
        mapped = jnp.dot(centred, pool_map[group_index], preferred_element_type=jnp.float32)
        outputs.append(mapped * pool_gain[group_index * HEAD:(group_index + 1) * HEAD].astype(jnp.float32))
    return jnp.concatenate(outputs, axis=1).astype(jnp.bfloat16)

def head_memory(inputs):
    query_rows, key_rows, value_rows, input_pre, log_forget = inputs
    blocks = SEQUENCE_TOKENS // BLOCK
    causal_mask = jnp.tril(jnp.ones((BLOCK, BLOCK), dtype=jnp.bool_))
    key_scale = HEAD ** (-0.5)

    def advance(carried_state, block_part):
        memory, peak_log = carried_state
        query_now, key_now, value_now, input_now, forget_now = block_part
        cumulative = jnp.cumsum(forget_now)
        block_total = cumulative[-1]
        log_diff = jnp.where(causal_mask, cumulative[:, None] - cumulative[None, :] + input_now[None, :], -jnp.inf)
        carry_log = cumulative + peak_log
        row_peak = jnp.maximum(lax.optimization_barrier(jnp.max(log_diff, axis=1)), carry_log)
        scores = jnp.dot(query_now, key_now.T, preferred_element_type=jnp.float32) * key_scale
        block_weights = (jnp.exp(log_diff - row_peak[:, None]) * scores).astype(jnp.bfloat16)
        within_block = jnp.dot(block_weights, value_now, preferred_element_type=jnp.float32)
        carried = jnp.dot(query_now.astype(jnp.float32), memory, precision=highest)
        carried = carried * jnp.exp(carry_log - row_peak)[:, None]
        hidden = within_block + carried
        along_log = block_total - cumulative + input_now
        new_peak = jnp.maximum(block_total + peak_log, jnp.max(along_log))
        scaled_keys = key_now.astype(jnp.float32) * (jnp.exp(along_log - new_peak) * key_scale)[:, None]
        memory = jnp.exp(block_total + peak_log - new_peak) * memory + jnp.dot(scaled_keys.T, value_now.astype(jnp.float32), precision=highest)
        return ((memory, new_peak), hidden)
    initial = (jnp.zeros((HEAD, HEAD), jnp.float32), jnp.zeros((), jnp.float32))
    stacked = (query_rows.reshape(blocks, BLOCK, HEAD), key_rows.reshape(blocks, BLOCK, HEAD), value_rows.reshape(blocks, BLOCK, HEAD), input_pre.reshape(blocks, BLOCK), log_forget.reshape(blocks, BLOCK))
    unused, hidden = lax.scan(advance, initial, stacked)
    return hidden.reshape(SEQUENCE_TOKENS, HEAD)

def by_head(array):
    return jnp.swapaxes(array.reshape(SEQUENCE_TOKENS, MEMORY_HEADS, HEAD), 0, 1)

def reference(tokens, norm_gain, w_pool_in, w_mem_in, w_input_gate, w_forget_gate, forget_bias, forget_extra, conv_weight, query_map, key_map, pool_map, pool_gain, mem_gain, w_out_pool, w_out_mem):
    normalized = rms_rows(tokens, norm_gain)
    pool_in = jnp.dot(normalized, w_pool_in, preferred_element_type=jnp.float32).astype(jnp.bfloat16)
    mem_in = jnp.dot(normalized, w_mem_in, preferred_element_type=jnp.float32).astype(jnp.bfloat16)
    input_pre = rounded(jnp.dot(normalized, w_input_gate, preferred_element_type=jnp.float32) * D ** (-0.5))
    forget_pre = rounded(jnp.dot(normalized, w_forget_gate, preferred_element_type=jnp.float32))
    log_forget = jax.nn.log_sigmoid(forget_pre + forget_bias) - forget_extra
    pool_mixed = pool_branch(pool_in, pool_map, pool_gain)
    padded = jnp.pad(mem_in.astype(jnp.float32), ((CONV - 1, 0), (0, 0)))
    conv_sum = padded[0:SEQUENCE_TOKENS] * conv_weight[0].astype(jnp.float32)
    for tap_index in range(1, CONV):
        conv_sum = conv_sum + padded[tap_index:tap_index + SEQUENCE_TOKENS] * conv_weight[tap_index].astype(jnp.float32)
    conv_in = jax.nn.silu(conv_sum).astype(jnp.bfloat16)
    conv_blocks = conv_in.astype(jnp.float32).reshape(SEQUENCE_TOKENS, MEM // 4, 4)
    query_rows = jnp.einsum('tnc,ncd->tnd', conv_blocks, query_map.astype(jnp.float32)).reshape(SEQUENCE_TOKENS, MEM).astype(jnp.bfloat16)
    key_rows = jnp.einsum('tnc,ncd->tnd', conv_blocks, key_map.astype(jnp.float32)).reshape(SEQUENCE_TOKENS, MEM).astype(jnp.bfloat16)
    hidden = lax.map(head_memory, (by_head(query_rows), by_head(key_rows), by_head(mem_in), input_pre.T, log_forget.T))
    hidden = jnp.swapaxes(hidden, 0, 1)
    centre = lax.optimization_barrier(jnp.mean(hidden, axis=-1, keepdims=True))
    spread_sq = lax.optimization_barrier(jnp.mean(jnp.square(hidden - centre), axis=-1, keepdims=True))
    normed = ((hidden - centre) * lax.rsqrt(spread_sq + epsilon)).reshape(SEQUENCE_TOKENS, MEM)
    mem_mixed = (normed * mem_gain.astype(jnp.float32)).astype(jnp.bfloat16)
    pool_run = POOL // N_TP
    mem_run = MEM // N_TP
    layer_out = jnp.zeros((SEQUENCE_TOKENS, D), jnp.float32)
    for member in range(N_TP):
        run_partial = jnp.dot(pool_mixed[:, member * pool_run:(member + 1) * pool_run], w_out_pool[member * pool_run:(member + 1) * pool_run], preferred_element_type=jnp.float32)
        run_partial = run_partial + jnp.dot(mem_mixed[:, member * mem_run:(member + 1) * mem_run], w_out_mem[member * mem_run:(member + 1) * mem_run], preferred_element_type=jnp.float32)
        layer_out = layer_out + rounded(run_partial)
    return layer_out.astype(jnp.bfloat16)
```

```python
import jax
import jax.numpy as jnp
from jax import lax
from jax.experimental import pallas as pl
from jax.experimental.pallas import tpu as pltpu
from jax.sharding import Mesh
from jax.sharding import PartitionSpec as P

D = 4096
HEAD = 256
CONV = 4
BLOCK = 128
MEMORY_HEADS = 16
SP = ("z", "y")
TP = ("x", "core")
SP_TP = ("z", "y", "x", "core")
RING = 4
GATE_LANES = 128
HALF_ROWS = 128

epsilon = 1e-06
windows_all = (2, 4, 8, 16)
highest = lax.Precision.HIGHEST
lowest = -1e30
f32 = jnp.float32
bf16 = jnp.bfloat16


def shifted(a, axis, by):
    n = lax.axis_size(axis)
    return lax.ppermute(a, axis, [(i, (i + by) % n) for i in range(n)])


def passed_along(shard, axis, by):
    devices = lax.axis_size(axis)
    pairs = [(i, i + by) for i in range(devices) if 0 <= i + by < devices]
    return lax.ppermute(shard, axis, pairs)


def gathered(shard, first, second):
    near = jnp.stack([shard, shifted(shard, first, 1)])
    far = jnp.stack([shifted(shard, first, 2), shifted(shard, first, -1)])
    near_up, far_down = shifted(near, second, 1), shifted(far, second, -1)
    far_up, near_down = shifted(far, second, 1), shifted(near, second, -1)
    return {
        (0, 0): near,
        (0, 1): far,
        (1, 0): near_up,
        (1, 1): far_up,
        (3, 0): near_down,
        (3, 1): far_down,
        (2, 0): shifted(near_up, second, 1),
        (2, 1): shifted(far_down, second, -1),
    }


def back(index, by):
    return lax.rem(index + (RING - by), RING)


def whole(shape):
    return pl.BlockSpec(shape, lambda: (0,) * len(shape))


def in_smem():
    return pl.BlockSpec(memory_space=pltpu.SMEM)


def params(mib):
    return pltpu.CompilerParams(vmem_limit_bytes=mib * 2**20)


def norm_rows(at, tokens, gain, w_input, w_forget):
    rows, width = tokens.shape

    def kernel(at_ref, tokens_ref, gain_ref, input_ref, forget_ref, out_ref, scratch):
        values = tokens_ref[...].astype(f32)
        factor = lax.rsqrt(jnp.mean(values * values, axis=-1, keepdims=True) + epsilon)
        normal = (values * factor * gain_ref[...].astype(f32)).astype(bf16)
        scratch[...] = normal
        to_input = jnp.dot(normal, input_ref[...], preferred_element_type=f32) * D ** (-0.5)
        to_forget = jnp.dot(normal, forget_ref[...], preferred_element_type=f32)
        spare = jnp.zeros((rows, GATE_LANES - 2 * MEMORY_HEADS), f32)
        gates = jnp.concatenate([to_input, to_forget, spare], axis=1)
        out_ref[:, width:] = gates.astype(bf16)
        z, y = at_ref[0], at_ref[1]
        for dz in range(RING):
            for dy in range(RING):
                block = back(z, dz) * RING + back(y, dy)
                start = pl.multiple_of(block * 2 * HALF_ROWS, 2 * HALF_ROWS)
                piece = scratch[:, pl.ds(start, 2 * HALF_ROWS)]
                first = (dz * RING + dy) * HALF_ROWS
                second = width // 2 + (dy * RING + dz) * HALF_ROWS
                out_ref[:, first : first + HALF_ROWS] = piece[:, :HALF_ROWS]
                out_ref[:, second : second + HALF_ROWS] = piece[:, HALF_ROWS:]

    return pl.pallas_call(
        kernel,
        out_shape=jax.ShapeDtypeStruct((rows, width + GATE_LANES), bf16),
        in_specs=[in_smem()] + [whole(a.shape) for a in (tokens, gain, w_input, w_forget)],
        out_specs=whole((rows, width + GATE_LANES)),
        scratch_shapes=[pltpu.VMEM((rows, width), bf16)],
        compiler_params=params(12),
        name="norm_rows",
    )(at, tokens, gain, w_input, w_forget)


PIECES = [(d2, half) for d2 in (0, 1, 3, 2) for half in range(2)]


def enter(rows_all, first, second, column):
    rows = rows_all.shape[0]
    cols = first[0, 0].shape[2] // 2
    buffers = [first[p] for p in PIECES] + [second[p] for p in PIECES]

    def kernel(rows_ref, *refs):
        out_ref = refs[-1]
        total = None
        for n, ref in enumerate(refs[:-1]):
            d2, half = PIECES[n % len(PIECES)]
            start = (n // len(PIECES)) * (D // 2) + (d2 * RING + 2 * half) * HALF_ROWS
            piece = ref[...].reshape(2 * HALF_ROWS, cols)
            part = jnp.dot(
                rows_ref[:, start : start + 2 * HALF_ROWS], piece, preferred_element_type=f32
            )
            total = part if total is None else total + part
        out_ref[...] = total.astype(bf16)

    return pl.pallas_call(
        kernel,
        grid=(1,),
        out_shape=jax.ShapeDtypeStruct((rows, cols), bf16),
        in_specs=[pl.BlockSpec(rows_all.shape, lambda i: (0, 0))]
        + [pl.BlockSpec((2, HALF_ROWS, cols), lambda i: (0, 0, column)) for _ in buffers],
        out_specs=pl.BlockSpec((rows, cols), lambda i: (0, 0)),
        compiler_params=params(24),
        name="enter_mem" if column == 0 else "enter_pool",
    )(rows_all, *buffers)


def leave(mixed, buffers):
    rows, depth = mixed.shape
    width = 2 * HALF_ROWS
    half = rows // 2

    def kernel(mixed_ref, *refs):
        own_ref, send_ref = refs[-2:]
        for n, ref in enumerate(refs[:-2]):
            pair = jnp.concatenate([ref[0], ref[1]], axis=1)
            part = jnp.dot(mixed_ref[...], pair, preferred_element_type=f32).astype(bf16)
            own_ref[:, n * width : (n + 1) * width] = part[:half]
            send_ref[:, n * width : (n + 1) * width] = part[half:]

    shape = (half, width * len(buffers))
    return pl.pallas_call(
        kernel,
        out_shape=(jax.ShapeDtypeStruct(shape, bf16), jax.ShapeDtypeStruct(shape, bf16)),
        in_specs=[whole(mixed.shape)] + [whole(b.shape) for b in buffers],
        out_specs=(whole(shape), whole(shape)),
        compiler_params=params(24),
        name="leave",
    )(mixed, *buffers)


def finish(at, groups, pieces):
    rows = groups[0][1].shape[0]
    flat = [a for group in groups for a in group]
    count = len(groups[0])

    def kernel(at_ref, *refs):
        out_ref = refs[-1]
        z, y = at_ref[0], at_ref[1]
        for g, kinds in enumerate(pieces):
            members = refs[g * count : (g + 1) * count]
            for n, (path, d2, half) in enumerate(kinds):
                for i in range(2):
                    d1 = 2 * half + i
                    dz, dy = (d2, d1) if path == 0 else (d1, d2)
                    block = back(z, dz) * RING + back(y, dy)
                    start = pl.multiple_of((2 * block + path) * HALF_ROWS, HALF_ROWS)
                    at_col = (2 * n + i) * HALF_ROWS
                    total = members[0][:rows, at_col : at_col + HALF_ROWS].astype(f32)
                    for member in members[1:]:
                        total = total + member[:, at_col : at_col + HALF_ROWS].astype(f32)
                    out_ref[:, pl.ds(start, HALF_ROWS)] = total.astype(bf16)

    return pl.pallas_call(
        kernel,
        out_shape=jax.ShapeDtypeStruct((rows, D), bf16),
        in_specs=[in_smem()] + [whole(a.shape) for a in flat],
        out_specs=whole((rows, D)),
        compiler_params=params(12),
        name="finish",
    )(at, *flat)


def first_peaks(at, logs, heads):
    devices = logs.shape[0]

    def kernel(at_ref, logs_ref, out_ref):
        for h in range(heads):
            peak = jnp.float32(0.0)
            for i in range(devices):
                joined = jnp.maximum(logs_ref[i, h] + peak, logs_ref[i, heads + h])
                peak = jnp.where(i < at_ref[2], joined, peak)
            out_ref[h] = peak

    return pl.pallas_call(
        kernel,
        out_shape=jax.ShapeDtypeStruct((heads,), f32),
        in_specs=[in_smem(), in_smem()],
        out_specs=in_smem(),
        name="first_peaks",
    )(at, logs)


def scan_states(logs, arrived):
    devices, heads, share, width = arrived.shape

    def kernel(logs_ref, arrived_ref, out_ref):
        for h in range(heads):
            state = jnp.zeros((share, width), f32)
            peak = jnp.float32(0.0)
            for i in range(devices):
                out_ref[i, h] = state
                decayed = logs_ref[i, h] + peak
                fresh = logs_ref[i, heads + h]
                joined = jnp.maximum(decayed, fresh)
                keep = jnp.exp(jnp.full((share, width), decayed - joined))
                add = jnp.exp(jnp.full((share, width), fresh - joined))
                state = keep * state + add * arrived_ref[i, h]
                peak = joined

    return pl.pallas_call(
        kernel,
        out_shape=jax.ShapeDtypeStruct(arrived.shape, f32),
        in_specs=[in_smem(), whole(arrived.shape)],
        out_specs=whole(arrived.shape),
        compiler_params=params(8),
        name="scan_states",
    )(logs, arrived)


def on_device(
    tokens,
    norm_gain,
    w_pool_in,
    w_mem_in,
    w_input_gate,
    w_forget_gate,
    forget_bias,
    forget_extra,
    conv_weight,
    query_map,
    key_map,
    pool_map,
    pool_gain,
    mem_gain,
    w_out_pool,
    w_out_mem,
):
    x_index = lax.axis_index("x")
    core_index = lax.axis_index("core")
    tp_index = lax.axis_index(TP)
    sp_index = lax.axis_index(SP)
    sp_size = lax.axis_size(SP)
    chips = lax.axis_size("x")
    own_rows = tokens.shape[0]
    seq_rows = own_rows * lax.axis_size(TP)
    group_count = pool_map.shape[0]
    pool_cols = group_count * HEAD
    head_count = forget_extra.shape[1]
    mem_cols = head_count * HEAD
    blocks = seq_rows // BLOCK

    at = jnp.stack([lax.axis_index("z"), lax.axis_index("y"), sp_index, x_index, core_index, tp_index])

    normalized = norm_rows(at, tokens, norm_gain.reshape(1, D), w_input_gate, w_forget_gate)
    width = normalized.shape[1]
    half = jnp.zeros((chips, own_rows, width), bf16)
    for k in range(chips):
        piece = normalized if k == 0 else shifted(normalized, "x", k)
        half = lax.dynamic_update_index_in_dim(half, piece, (x_index - k) % chips, 0)
    other = shifted(half, "core", 1)
    rows_all = jnp.zeros((chips, 2, own_rows, width), bf16)
    rows_all = lax.dynamic_update_index_in_dim(rows_all, half, core_index, 1)
    rows_all = lax.dynamic_update_index_in_dim(rows_all, other, 1 - core_index, 1)
    rows_all = rows_all.reshape(seq_rows, width)

    w_in = jnp.concatenate([w_mem_in, w_pool_in], axis=1)
    in_first = gathered(w_in[:HALF_ROWS], "y", "z")
    in_second = gathered(w_in[HALF_ROWS:], "z", "y")
    w_out = jnp.concatenate([w_out_pool, w_out_mem], axis=0)
    out_first = gathered(w_out[:, :HALF_ROWS], "y", "z")
    out_second = gathered(w_out[:, HALF_ROWS:], "z", "y")

    head_start = tp_index * head_count
    gate_rows = rows_all[:, D:]
    input_pre = lax.dynamic_slice_in_dim(gate_rows, head_start, head_count, 1).astype(f32)
    forget_pre = lax.dynamic_slice_in_dim(
        gate_rows, MEMORY_HEADS + head_start, head_count, 1
    ).astype(f32)
    bias_own = lax.dynamic_slice_in_dim(forget_bias, head_start, head_count, 0)
    log_forget = jax.nn.log_sigmoid(forget_pre + bias_own) - forget_extra
    forget_blocks = jnp.swapaxes(log_forget.reshape(blocks, BLOCK, head_count), 1, 2)
    input_blocks = jnp.swapaxes(input_pre.reshape(blocks, BLOCK, head_count), 1, 2)
    cumulative = jnp.cumsum(forget_blocks, axis=-1)
    block_total = cumulative[..., -1]
    along_log = block_total[..., None] - cumulative + input_blocks
    along_peak = jnp.max(along_log, axis=-1)
    key_weight = jnp.exp(along_log - along_peak[..., None]) * HEAD ** (-0.5)
    device_decay, device_peak = block_total[0], along_peak[0]
    decay_keep, decay_add = [None], [jnp.ones_like(device_peak)]
    for b in range(1, blocks):
        joined = jnp.maximum(block_total[b] + device_peak, along_peak[b])
        decay_keep.append(jnp.exp(block_total[b] + device_peak - joined))
        decay_add.append(jnp.exp(along_peak[b] - joined))
        device_decay, device_peak = device_decay + block_total[b], joined
    logs = jnp.concatenate([device_decay, device_peak, jnp.zeros((128 - 2 * head_count,), f32)])
    logs = jnp.broadcast_to(logs, (sp_size, 128))
    logs = lax.all_to_all(logs, SP, split_axis=0, concat_axis=0, tiled=True)
    start_peak = first_peaks(at, logs, head_count)
    block_peak, keep_blk, add_blk = [start_peak], [], []
    for b in range(blocks):
        joined = jnp.maximum(block_total[b] + block_peak[b], along_peak[b])
        keep_blk.append(jnp.exp(block_total[b] + block_peak[b] - joined))
        add_blk.append(jnp.exp(along_peak[b] - joined))
        block_peak.append(joined)
    block_peak = jnp.stack(block_peak[:blocks])
    causal_mask = jnp.tril(jnp.ones((BLOCK, BLOCK), dtype=jnp.bool_))
    log_diff = jnp.where(
        causal_mask,
        cumulative[..., :, None] - cumulative[..., None, :] + input_blocks[..., None, :],
        -jnp.inf,
    )
    carry_log = cumulative + block_peak[..., None]
    row_peak = jnp.maximum(jnp.max(log_diff, axis=-1), carry_log)

    mem_in = enter(rows_all, in_first, in_second, 0)
    mem_rim = passed_along(mem_in[seq_rows - (CONV - 1) :], SP, 1)
    mem_ext = jnp.concatenate([mem_rim, mem_in], axis=0).astype(f32)
    conv_own = lax.dynamic_slice_in_dim(conv_weight, tp_index * mem_cols, mem_cols, 1).astype(f32)
    conv_sum = mem_ext[0:seq_rows] * conv_own[0]
    for tap_index in range(1, CONV):
        conv_sum = conv_sum + mem_ext[tap_index : tap_index + seq_rows] * conv_own[tap_index]
    conv_in = jax.nn.silu(conv_sum).astype(bf16)

    def dense_map(map_table):
        own_blocks = lax.dynamic_slice_in_dim(
            map_table, tp_index * (mem_cols // 4), mem_cols // 4, 0
        ).reshape(mem_cols, 4)
        place = (jnp.arange(HEAD)[None, :] % 4 == jnp.arange(4)[:, None]).astype(bf16)
        spread = jnp.dot(own_blocks, place, preferred_element_type=f32)
        same = (jnp.arange(mem_cols)[:, None] % HEAD) // 4 == jnp.arange(HEAD)[None, :] // 4
        return jnp.where(same, spread, 0.0).astype(bf16).reshape(head_count, HEAD, HEAD)

    conv_heads = conv_in.reshape(seq_rows, head_count, HEAD)
    query_rows = jnp.einsum(
        "thc,hcd->thd", conv_heads, dense_map(query_map), preferred_element_type=f32
    ).astype(bf16)
    key_rows = jnp.einsum(
        "thc,hcd->thd", conv_heads, dense_map(key_map), preferred_element_type=f32
    ).astype(bf16)
    query_blocks = query_rows.reshape(blocks, BLOCK, head_count, HEAD)
    key_blocks = key_rows.reshape(blocks, BLOCK, head_count, HEAD)
    value_blocks = mem_in.reshape(blocks, BLOCK, head_count, HEAD)
    scaled_keys = key_blocks.astype(f32) * jnp.swapaxes(key_weight, 1, 2)[..., None]
    block_memory = jnp.einsum(
        "nlhd,nlhe->nhde", scaled_keys, value_blocks.astype(f32), precision=highest
    )
    device_memory = block_memory[0]
    for b in range(1, blocks):
        device_memory = (
            decay_keep[b][:, None, None] * device_memory
            + decay_add[b][:, None, None] * block_memory[b]
        )

    share = HEAD // sp_size
    pieces = jnp.moveaxis(device_memory.reshape(head_count, sp_size, share, HEAD), 1, 0)
    arrived = lax.all_to_all(pieces, SP, split_axis=0, concat_axis=0, tiled=True)
    starts = scan_states(logs, arrived)
    returned = lax.all_to_all(starts, SP, split_axis=0, concat_axis=0, tiled=True)
    state = jnp.moveaxis(returned, 0, 1).reshape(head_count, HEAD, HEAD)
    block_state = []
    for b in range(blocks):
        block_state.append(state)
        state = keep_blk[b][:, None, None] * state + add_blk[b][:, None, None] * block_memory[b]
    block_state = jnp.stack(block_state)

    scores = jnp.einsum(
        "nlhd,nshd->nhls", query_blocks, key_blocks, preferred_element_type=f32
    ) * HEAD ** (-0.5)
    block_weights = (jnp.exp(log_diff - row_peak[..., None]) * scores).astype(bf16)
    within_block = jnp.einsum(
        "nhls,nshe->nlhe", block_weights, value_blocks, preferred_element_type=f32
    )
    carried = jnp.einsum(
        "nlhd,nhde->nlhe", query_blocks.astype(f32), block_state, precision=highest
    )
    carried = carried * jnp.swapaxes(jnp.exp(carry_log - row_peak), 1, 2)[..., None]
    hidden = (within_block + carried).reshape(seq_rows, head_count, HEAD)
    centre = jnp.mean(hidden, axis=-1, keepdims=True)
    spread_sq = jnp.mean(jnp.square(hidden - centre), axis=-1, keepdims=True)
    normed = ((hidden - centre) * lax.rsqrt(spread_sq + epsilon)).reshape(seq_rows, mem_cols)
    mem_gain_own = lax.dynamic_slice_in_dim(mem_gain, tp_index * mem_cols, mem_cols, 0).astype(f32)
    mem_mixed = (normed * mem_gain_own).astype(bf16)

    pool_in = enter(rows_all, in_first, in_second, 1)
    pool_rim = passed_along(pool_in[seq_rows - 16 :], SP, 1)
    running = jnp.concatenate([pool_rim, pool_in], axis=0).astype(f32)
    stride_now = 1
    window_sums = []
    for window in windows_all:
        running = running[:-stride_now] + running[stride_now:]
        stride_now = window
        window_sums.append(running[17 - window : 17 - window + seq_rows])
    channel_group = tp_index * group_count + jnp.arange(pool_cols) // HEAD
    window_pick = channel_group % 4
    window_total = window_sums[0]
    for window_index in range(1, 4):
        window_total = jnp.where(
            window_pick == window_index, window_sums[window_index], window_total
        )
    window_len = (2 ** (window_pick + 1)).astype(f32)
    position = (sp_index * seq_rows + jnp.arange(seq_rows) + 1).astype(f32)
    counts = jnp.minimum(position[:, None], window_len[None, :])
    centred = (window_total / counts - pool_in.astype(f32)).astype(bf16)
    grouped = jnp.einsum(
        "tgc,gcd->tgd",
        centred.reshape(seq_rows, group_count, HEAD),
        pool_map,
        preferred_element_type=f32,
    )
    gain_own = lax.dynamic_slice_in_dim(pool_gain, tp_index * pool_cols, pool_cols, 0).astype(f32)
    pool_mixed = (grouped.reshape(seq_rows, pool_cols) * gain_own).astype(bf16)

    mixed = jnp.concatenate([pool_mixed, mem_mixed], axis=1)
    mixed = mixed.reshape(chips, 2, own_rows, pool_cols + mem_cols)
    mixed = lax.dynamic_slice_in_dim(jnp.concatenate([mixed, mixed], 0), x_index, chips, 0)
    mixed = lax.dynamic_slice_in_dim(jnp.concatenate([mixed, mixed], 1), core_index, 2, 1)
    mixed = jnp.swapaxes(mixed, 0, 1).reshape(seq_rows, pool_cols + mem_cols)
    groups, kinds = [], []
    for distances in ((0, 1, 3), (2,)):
        kinds.append([(path, d2, h) for path in range(2) for d2 in distances for h in range(2)])
        buffers = [(out_first, out_second)[path][d2, h] for path, d2, h in kinds[-1]]
        own, send = leave(mixed, buffers)
        came = shifted(send, "core", 1)
        pair = (own.astype(f32) + came.astype(f32)).astype(bf16)
        members = [pair]
        for k in range(1, chips):
            members.append(shifted(pair[k * own_rows : (k + 1) * own_rows], "x", k))
        groups.append(members)
    return finish(at, groups, kinds)


def solution(mesh):
    torus = Mesh(mesh.devices.reshape(4, 4, mesh.shape["tp"] // 2, 2), ("z", "y", "x", "core"))
    in_specs = (
        P(SP_TP, None),
        P(),
        P(SP, TP),
        P(SP, TP),
        P(),
        P(),
        P(),
        P(SP, TP),
        P(),
        P(),
        P(),
        P(TP, None, None),
        P(),
        P(),
        P(TP, SP),
        P(TP, SP),
    )
    out_specs = P(SP_TP, None)
    return jax.shard_map(
        on_device, mesh=torus, in_specs=in_specs, out_specs=out_specs, check_vma=False
    )
```

```python
import jax
import jax.numpy as jnp
from jax import lax
from jax.experimental import pallas as pl
from jax.experimental.pallas import tpu as pltpu
from jax.sharding import Mesh
from jax.sharding import PartitionSpec as P

D = 4096
HEAD = 256
CONV = 4
BLOCK = 128
MEMORY_HEADS = 16
SP = ("z", "y")
TP = ("x", "core")
SP_TP = ("z", "y", "x", "core")
RING = 4
GATE_LANES = 128
OUT_CHUNKS = 2
HALF_ROWS = 128

epsilon = 1e-06
f32 = jnp.float32
bf16 = jnp.bfloat16


def shifted(a, axis, by):
    n = lax.axis_size(axis)
    return lax.ppermute(a, axis, [(i, (i + by) % n) for i in range(n)])


def passed_along(shard, axis, by):
    devices = lax.axis_size(axis)
    pairs = [(i, i + by) for i in range(devices) if 0 <= i + by < devices]
    return lax.ppermute(shard, axis, pairs)


def first_phase(shard, axis):
    near = jnp.stack([shard, shifted(shard, axis, 1)])
    far = jnp.stack([shifted(shard, axis, 2), shifted(shard, axis, -1)])
    return near, far


def second_phase(near, far, axis):
    near_up, far_down = shifted(near, axis, 1), shifted(far, axis, -1)
    far_up, near_down = shifted(far, axis, 1), shifted(near, axis, -1)
    return {
        (0, 0): near,
        (0, 1): far,
        (1, 0): near_up,
        (1, 1): far_up,
        (3, 0): near_down,
        (3, 1): far_down,
        (2, 0): shifted(near_up, axis, 1),
        (2, 1): shifted(far_down, axis, -1),
    }


def back(index, by):
    return lax.rem(index + (RING - by), RING)


def whole(shape):
    return pl.BlockSpec(shape, lambda: (0,) * len(shape))


def in_smem():
    return pl.BlockSpec(memory_space=pltpu.SMEM)


def params(mib):
    return pltpu.CompilerParams(vmem_limit_bytes=mib * 2**20)


def norm_rows(at, tokens, gain, w_input, w_forget):
    rows, width = tokens.shape

    def kernel(at_ref, tokens_ref, gain_ref, input_ref, forget_ref, out_ref, scratch):
        values = tokens_ref[...].astype(f32)
        factor = lax.rsqrt(jnp.mean(values * values, axis=-1, keepdims=True) + epsilon)
        normal = (values * factor * gain_ref[...].astype(f32)).astype(bf16)
        scratch[...] = normal
        to_input = jnp.dot(normal, input_ref[...], preferred_element_type=f32) * D ** (-0.5)
        to_forget = jnp.dot(normal, forget_ref[...], preferred_element_type=f32)
        spare = jnp.zeros((rows, GATE_LANES - 2 * MEMORY_HEADS), f32)
        gates = jnp.concatenate([to_input, to_forget, spare], axis=1)
        out_ref[:, width:] = gates.astype(bf16)
        z, y = at_ref[0], at_ref[1]
        for dz in range(RING):
            for dy in range(RING):
                block = back(z, dz) * RING + back(y, dy)
                start = pl.multiple_of(block * 2 * HALF_ROWS, 2 * HALF_ROWS)
                piece = scratch[:, pl.ds(start, 2 * HALF_ROWS)]
                first = (dz * RING + dy) * HALF_ROWS
                second = width // 2 + (dy * RING + dz) * HALF_ROWS
                out_ref[:, first : first + HALF_ROWS] = piece[:, :HALF_ROWS]
                out_ref[:, second : second + HALF_ROWS] = piece[:, HALF_ROWS:]

    return pl.pallas_call(
        kernel,
        out_shape=jax.ShapeDtypeStruct((rows, width + GATE_LANES), bf16),
        in_specs=[in_smem()] + [whole(a.shape) for a in (tokens, gain, w_input, w_forget)],
        out_specs=whole((rows, width + GATE_LANES)),
        scratch_shapes=[pltpu.VMEM((rows, width), bf16)],
        compiler_params=params(12),
        name="norm_rows",
    )(at, tokens, gain, w_input, w_forget)


PIECES = [(d2, half) for d2 in (0, 1, 3, 2) for half in range(2)]


def enter(rows_all, first, second, name):
    rows = rows_all.shape[0]
    cols = first[0, 0].shape[2]
    buffers = [first[p] for p in PIECES] + [second[p] for p in PIECES]

    def kernel(rows_ref, *refs):
        out_ref = refs[-1]
        total = None
        for n, ref in enumerate(refs[:-1]):
            d2, half = PIECES[n % len(PIECES)]
            start = (n // len(PIECES)) * (D // 2) + (d2 * RING + 2 * half) * HALF_ROWS
            piece = ref[...].reshape(2 * HALF_ROWS, cols)
            part = jnp.dot(
                rows_ref[:, start : start + 2 * HALF_ROWS], piece, preferred_element_type=f32
            )
            total = part if total is None else total + part
        out_ref[...] = total.astype(bf16)

    return pl.pallas_call(
        kernel,
        out_shape=jax.ShapeDtypeStruct((rows, cols), bf16),
        in_specs=[whole(rows_all.shape)] + [whole(b.shape) for b in buffers],
        out_specs=whole((rows, cols)),
        compiler_params=params(24),
        name=name,
    )(rows_all, *buffers)


def square(shape):
    return lax.broadcasted_iota(jnp.int32, shape, 0), lax.broadcasted_iota(jnp.int32, shape, 1)


def log_sigmoid(v):
    return jnp.minimum(v, 0.0) - jnp.log1p(jnp.exp(-jnp.abs(v)))


def assemble(at, bias, extra, pieces, core_pieces):
    own_rows, width = pieces[0].shape
    chips = len(pieces)
    rows = 2 * chips * own_rows
    heads = extra.shape[1]

    def kernel(at_ref, bias_ref, extra_ref, *refs):
        sources, (rows_ref, col_ref, row_ref, logs_ref) = refs[: 2 * chips], refs[2 * chips :]
        x, core, tp = at_ref[3], at_ref[4], at_ref[5]
        for n, ref in enumerate(sources):
            owner = core if n < chips else 1 - core
            place = 2 * back(x, n % chips) + owner
            start = pl.multiple_of(place * own_rows, 16)
            rows_ref[pl.ds(start, own_rows), :] = ref[...]
        gates = rows_ref[:, width - GATE_LANES :].astype(f32)
        lane = lax.broadcasted_iota(jnp.int32, (BLOCK, GATE_LANES), 1)
        down, across = square((BLOCK, BLOCK))
        summary = jnp.zeros((8, GATE_LANES), f32)
        log_lane = lax.broadcasted_iota(jnp.int32, (8, GATE_LANES), 1)
        columns = [jnp.zeros((BLOCK, GATE_LANES), f32) for _ in range(rows // BLOCK)]
        row_ref[...] = jnp.zeros(row_ref.shape, f32)
        for h in range(heads):
            head = heads * tp + h
            decay, peak = None, None
            for b in range(rows // BLOCK):
                part = gates[b * BLOCK : (b + 1) * BLOCK]
                into = jnp.sum(jnp.where(lane == head, part, 0.0), axis=1, keepdims=True)
                keep = jnp.sum(
                    jnp.where(lane == MEMORY_HEADS + head, part, 0.0), axis=1, keepdims=True
                )
                log_keep = (
                    log_sigmoid(keep + bias_ref[head])
                    - extra_ref[b * BLOCK : (b + 1) * BLOCK, h : h + 1]
                )
                cum_row = jnp.sum(jnp.where(down <= across, log_keep, 0.0), axis=0, keepdims=True)
                cum_col = jnp.sum(jnp.where(down == across, cum_row, 0.0), axis=1, keepdims=True)
                into_row = jnp.sum(jnp.where(down == across, into, 0.0), axis=0, keepdims=True)
                columns[b] = jnp.where(lane == h, cum_col, columns[b])
                columns[b] = jnp.where(lane == heads + h, into, columns[b])
                row_ref[h : h + 1, b * BLOCK : (b + 1) * BLOCK] = cum_row
                row_ref[heads + h : heads + h + 1, b * BLOCK : (b + 1) * BLOCK] = into_row
                total = cum_row[:, BLOCK - 1 :]
                along = jnp.max(total - cum_row + into_row, axis=1, keepdims=True)
                if b == 0:
                    decay, peak = total, along
                else:
                    decay, peak = decay + total, jnp.maximum(total + peak, along)
            summary = jnp.where(log_lane == h, decay, summary)
            summary = jnp.where(log_lane == heads + h, peak, summary)
        for b in range(rows // BLOCK):
            col_ref[b * BLOCK : (b + 1) * BLOCK, :] = columns[b]
        logs_ref[...] = summary

    shapes = [((rows, width), bf16), ((rows, GATE_LANES), f32), ((8, rows), f32), ((8, GATE_LANES), f32)]
    return pl.pallas_call(
        kernel,
        out_shape=tuple(jax.ShapeDtypeStruct(s, t) for s, t in shapes),
        in_specs=[in_smem(), in_smem(), whole(extra.shape)]
        + [whole(a.shape) for a in (*pieces, *core_pieces)],
        out_specs=tuple(whole(s) for s, t in shapes),
        compiler_params=params(16),
        name="assemble",
    )(at, bias, extra, *pieces, *core_pieces)


def split_dot(a, b, contract, exact):
    wide = b if exact == 0 else a
    total = None
    for _ in range(3):
        part = wide.astype(bf16)
        wide = wide - part.astype(f32)
        pair = (a, part) if exact == 0 else (part, b)
        term = lax.dot_general(*pair, (contract, ((), ())), preferred_element_type=f32)
        total = term if total is None else total + term
    return total


def to_destinations(at_ref, source, out_ref, own_rows):
    x, core = at_ref[3], at_ref[4]
    for c in range(2):
        for k in range(RING):
            owner = core if c == 0 else 1 - core
            place = 2 * lax.rem(x + k, RING) + owner
            start = pl.multiple_of(place * own_rows, 16)
            first = (c * RING + k) * own_rows
            out_ref[first : first + own_rows, :] = source[pl.ds(start, own_rows), :]


def memory_before(at, logs, mem_in, rim, conv, query_dense, key_dense, col, row):
    rows, cols = mem_in.shape
    heads = cols // HEAD
    devices = logs.shape[0]
    share = HEAD // devices
    blocks = rows // BLOCK

    def kernel(
        at_ref, logs_ref, mem_ref, rim_ref, conv_ref, query_ref, key_ref, col_ref, row_ref,
        hidden_ref, rows_ref, weight_ref, own_ref, scratch,
    ):
        scratch[:8, :] = rim_ref[...].astype(f32)
        scratch[8:, :] = mem_ref[...].astype(f32)
        taps = conv_ref[...].astype(f32)
        total = scratch[9 - CONV : 9 - CONV + rows, :] * taps[0:1]
        for tap in range(1, CONV):
            first = 9 - CONV + tap
            total = total + scratch[first : first + rows, :] * taps[tap : tap + 1]
        conv_in = (total * lax.logistic(total)).astype(bf16)
        down, across = square((BLOCK, BLOCK))
        lane = lax.broadcasted_iota(jnp.int32, (BLOCK, GATE_LANES), 1)
        weights = [jnp.zeros((BLOCK, GATE_LANES), f32) for _ in range(blocks)]
        for h in range(heads):
            at_head = slice(h * HEAD, (h + 1) * HEAD)
            query = jnp.dot(conv_in[:, at_head], query_ref[h], preferred_element_type=f32).astype(bf16)
            key = jnp.dot(conv_in[:, at_head], key_ref[h], preferred_element_type=f32).astype(bf16)
            rows_ref[:, at_head] = query
            peak = jnp.float32(0.0)
            for i in range(devices):
                joined = jnp.maximum(logs_ref[i, h] + peak, logs_ref[i, heads + h])
                peak = jnp.where(i < at_ref[2], joined, peak)
            first_peak = jnp.full((1, 1), peak)
            now_peak, before = first_peak, jnp.zeros((1, 1), f32)
            own_peak, own, local = None, None, None
            for b in range(blocks):
                part = slice(b * BLOCK, (b + 1) * BLOCK)
                query_b, key_b, value_b = query[part], key[part], mem_ref[part, at_head]
                cum_col = col_ref[part, h : h + 1]
                into_col = col_ref[part, heads + h : heads + h + 1]
                cum_row, into_row = row_ref[h : h + 1, part], row_ref[heads + h : heads + h + 1, part]
                block_total = cum_row[:, BLOCK - 1 :]
                along_peak = jnp.max(block_total - cum_row + into_row, axis=1, keepdims=True)
                log_diff = jnp.where(across <= down, cum_col - cum_row + into_row, -jnp.inf)
                carry_log = cum_col + now_peak
                row_peak = jnp.maximum(jnp.max(log_diff, axis=1, keepdims=True), carry_log)
                scores = lax.dot_general(
                    query_b, key_b, (((1,), (1,)), ((), ())), preferred_element_type=f32
                ) * HEAD ** (-0.5)
                inside = (jnp.exp(log_diff - row_peak) * scores).astype(bf16)
                hidden = jnp.dot(inside, value_b, preferred_element_type=f32)
                if b:
                    carried = split_dot(query_b, local, ((1,), (0,)), 0)
                    hidden = hidden + carried * jnp.exp(carry_log - row_peak)
                hidden_ref[part, at_head] = hidden
                entering = jnp.exp(cum_col + before + first_peak - row_peak)
                weights[b] = jnp.where(lane == h, entering, weights[b])
                along_col = jnp.exp(block_total - cum_col + into_col - along_peak) * HEAD ** (-0.5)
                memory = split_dot(key_b.astype(f32) * along_col, value_b, ((0,), (0,)), 1)
                next_peak = jnp.maximum(block_total + now_peak, along_peak)
                fresh = jnp.exp(along_peak - next_peak) * memory
                if b == 0:
                    own, own_peak, local = memory, along_peak, fresh
                else:
                    joined = jnp.maximum(block_total + own_peak, along_peak)
                    own = (
                        jnp.exp(block_total + own_peak - joined) * own
                        + jnp.exp(along_peak - joined) * memory
                    )
                    own_peak = joined
                    local = jnp.exp(block_total + now_peak - next_peak) * local + fresh
                now_peak, before = next_peak, before + block_total
            for i in range(devices):
                own_ref[i, h] = own[i * share : (i + 1) * share]
        for b in range(blocks):
            weight_ref[b * BLOCK : (b + 1) * BLOCK, :] = weights[b]

    shapes = [
        ((rows, cols), f32),
        ((rows, cols), bf16),
        ((rows, GATE_LANES), f32),
        ((devices, heads, share, HEAD), f32),
    ]
    operands = (mem_in, rim, conv, query_dense, key_dense, col, row)
    return pl.pallas_call(
        kernel,
        out_shape=tuple(jax.ShapeDtypeStruct(s, t) for s, t in shapes),
        in_specs=[in_smem(), in_smem()] + [whole(a.shape) for a in operands],
        out_specs=tuple(whole(s) for s, t in shapes),
        scratch_shapes=[pltpu.VMEM((rows + 8, cols), f32)],
        compiler_params=params(16),
        name="memory_before",
    )(at, logs, *operands)


def memory_after(at, hidden, query, weight, states, gain, own_rows):
    rows, cols = hidden.shape
    heads = cols // HEAD

    def kernel(at_ref, hidden_ref, query_ref, weight_ref, states_ref, gain_ref, out_ref, scratch):
        for h in range(heads):
            at_head = slice(h * HEAD, (h + 1) * HEAD)
            state = states_ref[:, h].reshape(HEAD, HEAD)
            carried = split_dot(query_ref[:, at_head], state, ((1,), (0,)), 0)
            full = hidden_ref[:, at_head] + carried * weight_ref[:, h : h + 1]
            centre = jnp.mean(full, axis=-1, keepdims=True)
            spread = jnp.mean(jnp.square(full - centre), axis=-1, keepdims=True)
            normal = (full - centre) * lax.rsqrt(spread + epsilon)
            scratch[:, at_head] = (normal * gain_ref[:, at_head].astype(f32)).astype(bf16)
        to_destinations(at_ref, scratch, out_ref, own_rows)

    operands = (hidden, query, weight, states, gain)
    return pl.pallas_call(
        kernel,
        out_shape=jax.ShapeDtypeStruct((rows, cols), bf16),
        in_specs=[in_smem()] + [whole(a.shape) for a in operands],
        out_specs=whole((rows, cols)),
        scratch_shapes=[pltpu.VMEM((rows, cols), bf16)],
        compiler_params=params(16),
        name="memory_after",
    )(at, *operands)


def pooling(at, pool_in, rim, pool_map, gain, own_rows):
    rows, cols = pool_in.shape
    groups = cols // HEAD
    lead, reach = 8, rim.shape[0]

    def kernel(at_ref, pool_ref, rim_ref, map_ref, gain_ref, out_ref, sums, scratch):
        sp, tp = at_ref[2], at_ref[5]
        late = lax.rem(groups * tp, 4) >= 2
        end = lead + reach + rows
        time = lax.broadcasted_iota(jnp.int32, (rows, 1), 0) + sp * rows + 1
        for g in range(groups):
            at_group = slice(g * HEAD, (g + 1) * HEAD)
            values = pool_ref[:, at_group].astype(f32)
            for n in range(4):
                sums[n, :lead, :] = jnp.zeros((lead, HEAD), f32)
            sums[0, lead : lead + reach, :] = rim_ref[:, at_group].astype(f32)
            sums[0, lead + reach :, :] = values
            steps = 3 if g == 0 else 4
            for n in range(1, steps):
                by = 2 ** (n - 1)
                sums[n, lead:, :] = sums[n - 1, lead:, :] + sums[n - 1, lead - by : end - by, :]
            start = lead + reach
            if g == 0:
                by = 4
                longer = sums[2, start:, :] + sums[2, start - by : end - by, :]
                shorter = sums[1, start:, :]
            else:
                by = 8
                longer = sums[3, start:, :] + sums[3, start - by : end - by, :]
                shorter = sums[2, start:, :]
            window = jnp.where(late, 8 if g == 0 else 16, 2 if g == 0 else 4)
            count = jnp.minimum(time, window).astype(f32)
            centred = (jnp.where(late, longer, shorter) / count - values).astype(bf16)
            mixed = jnp.dot(centred, map_ref[g], preferred_element_type=f32)
            scratch[:, at_group] = (mixed * gain_ref[:, at_group].astype(f32)).astype(bf16)
        to_destinations(at_ref, scratch, out_ref, own_rows)

    operands = (pool_in, rim, pool_map, gain)
    return pl.pallas_call(
        kernel,
        out_shape=jax.ShapeDtypeStruct((rows, cols), bf16),
        in_specs=[in_smem()] + [whole(a.shape) for a in operands],
        out_specs=whole((rows, cols)),
        scratch_shapes=[
            pltpu.VMEM((4, lead + reach + rows, HEAD), f32),
            pltpu.VMEM((rows, cols), bf16),
        ],
        compiler_params=params(16),
        name="pooling",
    )(at, *operands)


def leave(pool_mixed, mem_mixed, weights, first, count):
    rows, pool_cols = pool_mixed.shape
    mem_cols = mem_mixed.shape[1]
    width = weights.shape[2]
    half = rows // 2
    step = 2

    def kernel(pool_ref, mem_ref, weight_ref, own_ref, send_ref):
        for n in range(step):
            part = jnp.dot(pool_ref[...], weight_ref[n, :pool_cols], preferred_element_type=f32)
            part = part + jnp.dot(mem_ref[...], weight_ref[n, pool_cols:], preferred_element_type=f32)
            part = part.astype(bf16)
            own_ref[:, n * width : (n + 1) * width] = part[:half]
            send_ref[:, n * width : (n + 1) * width] = part[half:]

    shape = (half, width * count)
    out_spec = pl.BlockSpec((half, width * step), lambda i: (0, i))
    return pl.pallas_call(
        kernel,
        grid=(count // step,),
        out_shape=(jax.ShapeDtypeStruct(shape, bf16), jax.ShapeDtypeStruct(shape, bf16)),
        in_specs=[
            pl.BlockSpec((rows, pool_cols), lambda i: (0, 0)),
            pl.BlockSpec((rows, mem_cols), lambda i: (0, 0)),
            pl.BlockSpec((step, pool_cols + mem_cols, width), lambda i: (first // step + i, 0, 0)),
        ],
        out_specs=(out_spec, out_spec),
        compiler_params=params(16),
        name="leave",
    )(pool_mixed, mem_mixed, weights)


def scan_states(logs, arrived):
    devices, heads, share, width = arrived.shape

    def kernel(logs_ref, arrived_ref, out_ref):
        for h in range(heads):
            state = jnp.zeros((share, width), f32)
            peak = jnp.float32(0.0)
            for i in range(devices):
                out_ref[i, h] = state
                decayed = logs_ref[i, h] + peak
                fresh = logs_ref[i, heads + h]
                joined = jnp.maximum(decayed, fresh)
                keep = jnp.exp(jnp.full((share, width), decayed - joined))
                add = jnp.exp(jnp.full((share, width), fresh - joined))
                state = keep * state + add * arrived_ref[i, h]
                peak = joined

    return pl.pallas_call(
        kernel,
        out_shape=jax.ShapeDtypeStruct(arrived.shape, f32),
        in_specs=[in_smem(), whole(arrived.shape)],
        out_specs=whole(arrived.shape),
        compiler_params=params(8),
        name="scan_states",
    )(logs, arrived)


def on_device(
    tokens,
    norm_gain,
    w_pool_in,
    w_mem_in,
    w_input_gate,
    w_forget_gate,
    forget_bias,
    forget_extra,
    conv_weight,
    query_map,
    key_map,
    pool_map,
    pool_gain,
    mem_gain,
    w_out_pool,
    w_out_mem,
):
    x_index = lax.axis_index("x")
    core_index = lax.axis_index("core")
    tp_index = lax.axis_index(TP)
    sp_index = lax.axis_index(SP)
    sp_size = lax.axis_size(SP)
    chips = lax.axis_size("x")
    own_rows = tokens.shape[0]
    seq_rows = own_rows * lax.axis_size(TP)
    group_count = pool_map.shape[0]
    pool_cols = group_count * HEAD
    head_count = forget_extra.shape[1]
    mem_cols = head_count * HEAD
    blocks = seq_rows // BLOCK

    at = jnp.stack([lax.axis_index("z"), lax.axis_index("y"), sp_index, x_index, core_index, tp_index])
    pool_at, mem_at = tp_index * pool_cols, tp_index * mem_cols

    w_out = lax.all_gather(
        jnp.concatenate([w_out_pool, w_out_mem], axis=0), SP, axis=0, tiled=False
    )

    w_in = jnp.concatenate([w_mem_in, w_pool_in], axis=1)
    rings = [("y", "z"), ("z", "y")]
    phase = [
        first_phase(w_in[n * HALF_ROWS : (n + 1) * HALF_ROWS], rings[n][0]) for n in range(2)
    ]
    cut = w_mem_in.shape[1]
    w_mem = [second_phase(*(a[..., :cut] for a in phase[n]), rings[n][1]) for n in range(2)]
    w_pool = [second_phase(*(a[..., cut:] for a in phase[n]), rings[n][1]) for n in range(2)]

    normalized = norm_rows(at, tokens, norm_gain.reshape(1, D), w_input_gate, w_forget_gate)
    pieces = [normalized] + [shifted(normalized, "x", k) for k in range(1, chips)]
    core_pieces = [shifted(piece, "core", 1) for piece in pieces]
    rows_all, col, row, logs = assemble(at, forget_bias, forget_extra, pieces, core_pieces)
    logs = jnp.broadcast_to(logs[:1], (sp_size, GATE_LANES))
    logs = lax.all_to_all(logs, SP, split_axis=0, concat_axis=0, tiled=True)

    def dense_map(map_table):
        own_blocks = lax.dynamic_slice_in_dim(map_table, mem_at // 4, mem_cols // 4, 0)
        own_blocks = own_blocks.reshape(mem_cols, 4)
        place = (jnp.arange(HEAD)[None, :] % 4 == jnp.arange(4)[:, None]).astype(bf16)
        spread = jnp.dot(own_blocks, place, preferred_element_type=f32)
        same = (jnp.arange(mem_cols)[:, None] % HEAD) // 4 == jnp.arange(HEAD)[None, :] // 4
        return jnp.where(same, spread, 0.0).astype(bf16).reshape(head_count, HEAD, HEAD)

    conv_own = lax.dynamic_slice_in_dim(conv_weight, mem_at, mem_cols, 1)
    mem_in = enter(rows_all, *w_mem, "enter_mem")
    mem_rim = passed_along(mem_in[seq_rows - 8 :], SP, 1)
    hidden, query, weight, own_state = memory_before(
        at, logs, mem_in, mem_rim, conv_own, dense_map(query_map), dense_map(key_map), col, row
    )
    arrived = lax.all_to_all(own_state, SP, split_axis=0, concat_axis=0, tiled=True)
    starts = scan_states(logs, arrived)
    states = lax.all_to_all(starts, SP, split_axis=0, concat_axis=0, tiled=True)
    mem_gain_own = lax.dynamic_slice_in_dim(mem_gain, mem_at, mem_cols, 0).reshape(1, mem_cols)
    mem_mixed = memory_after(at, hidden, query, weight, states, mem_gain_own, own_rows)

    pool_in = enter(rows_all, *w_pool, "enter_pool")
    pool_rim = passed_along(pool_in[seq_rows - 16 :], SP, 1)
    pool_gain_own = lax.dynamic_slice_in_dim(pool_gain, pool_at, pool_cols, 0).reshape(1, pool_cols)
    pool_mixed = pooling(at, pool_in, pool_rim, pool_map, pool_gain_own, own_rows)

    outs = []
    for n in range(OUT_CHUNKS):
        count = sp_size // OUT_CHUNKS
        own, send = leave(pool_mixed, mem_mixed, w_out, n * count, count)
        came = shifted(send, "core", 1)
        pair = (own.astype(f32) + came.astype(f32)).astype(bf16)
        total = pair[:own_rows].astype(f32)
        for k in range(1, chips):
            total = total + shifted(pair[k * own_rows : (k + 1) * own_rows], "x", k).astype(f32)
        outs.append(total.astype(bf16))
    return jnp.concatenate(outs, axis=1)


def solution(mesh):
    torus = Mesh(mesh.devices.reshape(4, 4, mesh.shape["tp"] // 2, 2), ("z", "y", "x", "core"))
    in_specs = (
        P(SP_TP, None),
        P(),
        P(SP, TP),
        P(SP, TP),
        P(),
        P(),
        P(),
        P(SP, TP),
        P(),
        P(),
        P(),
        P(TP, None, None),
        P(),
        P(),
        P(TP, SP),
        P(TP, SP),
    )
    out_specs = P(SP_TP, None)
    return jax.shard_map(
        on_device, mesh=torus, in_specs=in_specs, out_specs=out_specs, check_vma=False
    )
```

```python
import jax
import jax.numpy as jnp
from jax import lax
from jax.experimental import pallas as pl
from jax.experimental.pallas import tpu as pltpu
from jax.sharding import Mesh
from jax.sharding import PartitionSpec as P

D = 4096
HEAD = 256
CONV = 4
BLOCK = 128
MEMORY_HEADS = 16
SP = ("z", "y")
TP = ("x", "core")
SP_TP = ("z", "y", "x", "core")
RING = 4
GATE_LANES = 128
OUT_CHUNKS = 2
HALF_ROWS = 128


epsilon = 1e-06
f32 = jnp.float32
bf16 = jnp.bfloat16


def shifted(a, axis, by):
    n = lax.axis_size(axis)
    return lax.ppermute(a, axis, [(i, (i + by) % n) for i in range(n)])


def passed_along(shard, axis, by):
    devices = lax.axis_size(axis)
    pairs = [(i, i + by) for i in range(devices) if 0 <= i + by < devices]
    return lax.ppermute(shard, axis, pairs)


def first_phase(shard, axis):
    near = jnp.stack([shard, shifted(shard, axis, 1)])
    far = jnp.stack([shifted(shard, axis, 2), shifted(shard, axis, -1)])
    return near, far


def second_phase(near, far, axis):
    near_up, far_down = shifted(near, axis, 1), shifted(far, axis, -1)
    far_up, near_down = shifted(far, axis, 1), shifted(near, axis, -1)
    return {
        (0, 0): near,
        (0, 1): far,
        (1, 0): near_up,
        (1, 1): far_up,
        (3, 0): near_down,
        (3, 1): far_down,
        (2, 0): shifted(near_up, axis, 1),
        (2, 1): shifted(far_down, axis, -1),
    }


def back(index, by):
    return lax.rem(index + (RING - by), RING)


def whole(shape):
    return pl.BlockSpec(shape, lambda: (0,) * len(shape))


def in_smem():
    return pl.BlockSpec(memory_space=pltpu.SMEM)


def params(mib):
    return pltpu.CompilerParams(vmem_limit_bytes=mib * 2**20)


def norm_rows(at, tokens, gain, w_input, w_forget):
    rows, width = tokens.shape

    def kernel(at_ref, tokens_ref, gain_ref, input_ref, forget_ref, out_ref, scratch):
        values = tokens_ref[...].astype(f32)
        factor = lax.rsqrt(jnp.mean(values * values, axis=-1, keepdims=True) + epsilon)
        normal = (values * factor * gain_ref[...].astype(f32)).astype(bf16)
        scratch[...] = normal
        to_input = jnp.dot(normal, input_ref[...], preferred_element_type=f32) * D ** (-0.5)
        to_forget = jnp.dot(normal, forget_ref[...], preferred_element_type=f32)
        spare = jnp.zeros((rows, GATE_LANES - 2 * MEMORY_HEADS), f32)
        gates = jnp.concatenate([to_input, to_forget, spare], axis=1)
        out_ref[:, width:] = gates.astype(bf16)
        z, y = at_ref[0], at_ref[1]
        for dz in range(RING):
            for dy in range(RING):
                block = back(z, dz) * RING + back(y, dy)
                start = pl.multiple_of(block * 2 * HALF_ROWS, 2 * HALF_ROWS)
                piece = scratch[:, pl.ds(start, 2 * HALF_ROWS)]
                first = (dz * RING + dy) * HALF_ROWS
                second = width // 2 + (dy * RING + dz) * HALF_ROWS
                out_ref[:, first : first + HALF_ROWS] = piece[:, :HALF_ROWS]
                out_ref[:, second : second + HALF_ROWS] = piece[:, HALF_ROWS:]

    return pl.pallas_call(
        kernel,
        out_shape=jax.ShapeDtypeStruct((rows, width + GATE_LANES), bf16),
        in_specs=[in_smem()] + [whole(a.shape) for a in (tokens, gain, w_input, w_forget)],
        out_specs=whole((rows, width + GATE_LANES)),
        scratch_shapes=[pltpu.VMEM((rows, width), bf16)],
        compiler_params=params(12),
        name="norm_rows",
    )(at, tokens, gain, w_input, w_forget)


PIECES = [(d2, half) for d2 in (0, 1, 3, 2) for half in range(2)]


def enter(rows_all, first, second, rim_rows, name):
    rows = rows_all.shape[0]
    cols = first[0, 0].shape[2]
    buffers = [first[p] for p in PIECES] + [second[p] for p in PIECES]
    count = len(buffers)

    def kernel(rows_ref, *refs):
        out_ref, rim_ref, held, sems = refs[count:]
        copies = [
            pltpu.make_async_copy(refs[n], held.at[n], sems.at[n]) for n in range(count)
        ]
        for copy in copies:
            copy.start()
        total = None
        for n in range(count):
            copies[n].wait()
            d2, half = PIECES[n % len(PIECES)]
            start = (n // len(PIECES)) * (D // 2) + (d2 * RING + 2 * half) * HALF_ROWS
            part = jnp.dot(
                rows_ref[:, start : start + 2 * HALF_ROWS],
                held[n].reshape(2 * HALF_ROWS, cols),
                preferred_element_type=f32,
            )
            total = part if total is None else total + part
        total = total.astype(bf16)
        out_ref[...] = total
        rim_ref[...] = total[rows - rim_rows :]

    shapes = [(rows, cols), (rim_rows, cols)]
    return pl.pallas_call(
        kernel,
        out_shape=tuple(jax.ShapeDtypeStruct(s, bf16) for s in shapes),
        in_specs=[whole(rows_all.shape)] + [pl.BlockSpec(memory_space=pl.ANY)] * count,
        out_specs=tuple(whole(s) for s in shapes),
        scratch_shapes=[
            pltpu.VMEM((count, *buffers[0].shape), bf16),
            pltpu.SemaphoreType.DMA((count,)),
        ],
        compiler_params=params(24),
        name=name,
    )(rows_all, *buffers)


def square(shape):
    return lax.broadcasted_iota(jnp.int32, shape, 0), lax.broadcasted_iota(jnp.int32, shape, 1)


def log_sigmoid(v):
    return jnp.minimum(v, 0.0) - jnp.log1p(jnp.exp(-jnp.abs(v)))


def assemble(at, bias, extra, pieces, core_pieces):
    own_rows, width = pieces[0].shape
    chips = len(pieces)
    rows = 2 * chips * own_rows
    heads = extra.shape[1]

    def kernel(at_ref, bias_ref, extra_ref, *refs):
        sources, (rows_ref, col_ref, row_ref, logs_ref) = refs[: 2 * chips], refs[2 * chips :]
        x, core, tp = at_ref[3], at_ref[4], at_ref[5]
        for n, ref in enumerate(sources):
            owner = core if n < chips else 1 - core
            place = 2 * back(x, n % chips) + owner
            start = pl.multiple_of(place * own_rows, 16)
            rows_ref[pl.ds(start, own_rows), :] = ref[...]
        gates = rows_ref[:, width - GATE_LANES :].astype(f32)
        lane = lax.broadcasted_iota(jnp.int32, (BLOCK, GATE_LANES), 1)
        down, across = square((BLOCK, BLOCK))
        summary = jnp.zeros((8, GATE_LANES), f32)
        log_lane = lax.broadcasted_iota(jnp.int32, (8, GATE_LANES), 1)
        columns = [jnp.zeros((BLOCK, GATE_LANES), f32) for _ in range(rows // BLOCK)]
        row_ref[...] = jnp.zeros(row_ref.shape, f32)
        for h in range(heads):
            head = heads * tp + h
            decay, peak = None, None
            for b in range(rows // BLOCK):
                part = gates[b * BLOCK : (b + 1) * BLOCK]
                into = jnp.sum(jnp.where(lane == head, part, 0.0), axis=1, keepdims=True)
                keep = jnp.sum(
                    jnp.where(lane == MEMORY_HEADS + head, part, 0.0), axis=1, keepdims=True
                )
                log_keep = (
                    log_sigmoid(keep + bias_ref[head])
                    - extra_ref[b * BLOCK : (b + 1) * BLOCK, h : h + 1]
                )
                cum_row = jnp.sum(jnp.where(down <= across, log_keep, 0.0), axis=0, keepdims=True)
                cum_col = jnp.sum(jnp.where(down == across, cum_row, 0.0), axis=1, keepdims=True)
                into_row = jnp.sum(jnp.where(down == across, into, 0.0), axis=0, keepdims=True)
                columns[b] = jnp.where(lane == h, cum_col, columns[b])
                columns[b] = jnp.where(lane == heads + h, into, columns[b])
                row_ref[h : h + 1, b * BLOCK : (b + 1) * BLOCK] = cum_row
                row_ref[heads + h : heads + h + 1, b * BLOCK : (b + 1) * BLOCK] = into_row
                total = cum_row[:, BLOCK - 1 :]
                along = jnp.max(total - cum_row + into_row, axis=1, keepdims=True)
                if b == 0:
                    decay, peak = total, along
                else:
                    decay, peak = decay + total, jnp.maximum(total + peak, along)
            summary = jnp.where(log_lane == h, decay, summary)
            summary = jnp.where(log_lane == heads + h, peak, summary)
        for b in range(rows // BLOCK):
            col_ref[b * BLOCK : (b + 1) * BLOCK, :] = columns[b]
        logs_ref[...] = summary

    shapes = [((rows, width), bf16), ((rows, GATE_LANES), f32), ((8, rows), f32), ((8, GATE_LANES), f32)]
    return pl.pallas_call(
        kernel,
        out_shape=tuple(jax.ShapeDtypeStruct(s, t) for s, t in shapes),
        in_specs=[in_smem(), in_smem(), whole(extra.shape)]
        + [whole(a.shape) for a in (*pieces, *core_pieces)],
        out_specs=tuple(whole(s) for s, t in shapes),
        compiler_params=params(16),
        name="assemble",
    )(at, bias, extra, *pieces, *core_pieces)


def split_dot(a, b, contract, exact):
    wide = b if exact == 0 else a
    total = None
    for _ in range(3):
        part = wide.astype(bf16)
        wide = wide - part.astype(f32)
        pair = (a, part) if exact == 0 else (part, b)
        term = lax.dot_general(*pair, (contract, ((), ())), preferred_element_type=f32)
        total = term if total is None else total + term
    return total


def to_destinations(at_ref, source, out_ref, own_rows):
    x, core = at_ref[3], at_ref[4]
    for c in range(2):
        for k in range(RING):
            owner = core if c == 0 else 1 - core
            place = 2 * lax.rem(x + k, RING) + owner
            start = pl.multiple_of(place * own_rows, 16)
            first = (c * RING + k) * own_rows
            out_ref[first : first + own_rows, :] = source[pl.ds(start, own_rows), :]


def memory_before(devices, logs, mem_in, rim, conv, query_dense, key_dense, col, row):
    rows, cols = mem_in.shape
    heads = cols // HEAD
    share = HEAD // devices
    blocks = rows // BLOCK

    def kernel(
        logs_ref, mem_ref, rim_ref, conv_ref, query_ref, key_ref, col_ref, row_ref,
        hidden_ref, rows_ref, weight_ref, own_ref, scratch,
    ):
        scratch[:8, :] = rim_ref[...].astype(f32)
        scratch[8:, :] = mem_ref[...].astype(f32)
        taps = conv_ref[...].astype(f32)
        total = scratch[9 - CONV : 9 - CONV + rows, :] * taps[0:1]
        for tap in range(1, CONV):
            first = 9 - CONV + tap
            total = total + scratch[first : first + rows, :] * taps[tap : tap + 1]
        conv_in = (total * lax.logistic(total)).astype(bf16)
        down, across = square((BLOCK, BLOCK))
        lane = lax.broadcasted_iota(jnp.int32, (BLOCK, GATE_LANES), 1)
        weights = [jnp.zeros((BLOCK, GATE_LANES), f32) for _ in range(blocks)]
        for h in range(heads):
            at_head = slice(h * HEAD, (h + 1) * HEAD)
            query = jnp.dot(conv_in[:, at_head], query_ref[h], preferred_element_type=f32).astype(bf16)
            key = jnp.dot(conv_in[:, at_head], key_ref[h], preferred_element_type=f32).astype(bf16)
            rows_ref[:, at_head] = query
            before = jnp.zeros((1, 1), f32)
            own_peak, own = None, None
            for b in range(blocks):
                part = slice(b * BLOCK, (b + 1) * BLOCK)
                query_b, key_b, value_b = query[part], key[part], mem_ref[part, at_head]
                cum_col = col_ref[part, h : h + 1]
                into_col = col_ref[part, heads + h : heads + h + 1]
                cum_row, into_row = row_ref[h : h + 1, part], row_ref[heads + h : heads + h + 1, part]
                block_total = cum_row[:, BLOCK - 1 :]
                along_peak = jnp.max(block_total - cum_row + into_row, axis=1, keepdims=True)
                log_diff = jnp.where(across <= down, cum_col - cum_row + into_row, -jnp.inf)
                row_peak = jnp.max(log_diff, axis=1, keepdims=True)
                if b:
                    carry_log = cum_col + own_peak
                    row_peak = jnp.maximum(row_peak, carry_log)
                scores = lax.dot_general(
                    query_b, key_b, (((1,), (1,)), ((), ())), preferred_element_type=f32
                ) * HEAD ** (-0.5)
                inside = (jnp.exp(log_diff - row_peak) * scores).astype(bf16)
                hidden = jnp.dot(inside, value_b, preferred_element_type=f32)
                if b:
                    carried = split_dot(query_b, own, ((1,), (0,)), 0)
                    hidden = hidden + carried * jnp.exp(carry_log - row_peak)
                hidden_ref[part, at_head] = hidden
                weights[b] = jnp.where(lane == h, row_peak, weights[b])
                weights[b] = jnp.where(lane == heads + h, cum_col + before, weights[b])
                along_col = jnp.exp(block_total - cum_col + into_col - along_peak) * HEAD ** (-0.5)
                memory = split_dot(key_b.astype(f32) * along_col, value_b, ((0,), (0,)), 1)
                if b == 0:
                    own, own_peak = memory, along_peak
                else:
                    joined = jnp.maximum(block_total + own_peak, along_peak)
                    own = (
                        jnp.exp(block_total + own_peak - joined) * own
                        + jnp.exp(along_peak - joined) * memory
                    )
                    own_peak = joined
                before = before + block_total
            for i in range(devices):
                own_ref[i, h * share : (h + 1) * share] = own[i * share : (i + 1) * share]
        for b in range(blocks):
            weight_ref[b * BLOCK : (b + 1) * BLOCK, :] = weights[b]
        for i in range(devices):
            own_ref[i, heads * share :, :GATE_LANES] = logs_ref[...]
            own_ref[i, heads * share :, GATE_LANES:] = jnp.zeros((8, HEAD - GATE_LANES), f32)

    shapes = [
        ((rows, cols), f32),
        ((rows, cols), bf16),
        ((rows, GATE_LANES), f32),
        ((devices, heads * share + 8, HEAD), f32),
    ]
    operands = (logs, mem_in, rim, conv, query_dense, key_dense, col, row)
    return pl.pallas_call(
        kernel,
        out_shape=tuple(jax.ShapeDtypeStruct(s, t) for s, t in shapes),
        in_specs=[whole(a.shape) for a in operands],
        out_specs=tuple(whole(s) for s, t in shapes),
        scratch_shapes=[pltpu.VMEM((rows + 8, cols), f32)],
        compiler_params=params(16),
        name="memory_before",
    )(*operands)


def memory_after(at, hidden, query, weight, states, peaks, gain, own_rows):
    rows, cols = hidden.shape
    heads = cols // HEAD

    def kernel(at_ref, hidden_ref, query_ref, weight_ref, states_ref, peaks_ref, gain_ref, out_ref, scratch):
        for h in range(heads):
            at_head = slice(h * HEAD, (h + 1) * HEAD)
            state = states_ref[:, h].reshape(HEAD, HEAD)
            carried = split_dot(query_ref[:, at_head], state, ((1,), (0,)), 0)
            inner = weight_ref[:, h : h + 1]
            outer = weight_ref[:, heads + h : heads + h + 1] + peaks_ref[:1, h : h + 1]
            peak = jnp.maximum(inner, outer)
            full = hidden_ref[:, at_head] * jnp.exp(inner - peak) + carried * jnp.exp(outer - peak)
            centre = jnp.mean(full, axis=-1, keepdims=True)
            spread = jnp.mean(jnp.square(full - centre), axis=-1, keepdims=True)
            normal = (full - centre) * lax.rsqrt(spread + epsilon)
            scratch[:, at_head] = (normal * gain_ref[:, at_head].astype(f32)).astype(bf16)
        to_destinations(at_ref, scratch, out_ref, own_rows)

    operands = (hidden, query, weight, states, peaks, gain)
    return pl.pallas_call(
        kernel,
        out_shape=jax.ShapeDtypeStruct((rows, cols), bf16),
        in_specs=[in_smem()] + [whole(a.shape) for a in operands],
        out_specs=whole((rows, cols)),
        scratch_shapes=[pltpu.VMEM((rows, cols), bf16)],
        compiler_params=params(16),
        name="memory_after",
    )(at, *operands)


def pooling(at, pool_in, rim, pool_map, gain, own_rows):
    rows, cols = pool_in.shape
    groups = cols // HEAD
    lead, reach = 8, rim.shape[0]

    def kernel(at_ref, pool_ref, rim_ref, map_ref, gain_ref, out_ref, sums, scratch):
        sp, tp = at_ref[2], at_ref[5]
        late = lax.rem(groups * tp, 4) >= 2
        end = lead + reach + rows
        time = lax.broadcasted_iota(jnp.int32, (rows, 1), 0) + sp * rows + 1
        for g in range(groups):
            at_group = slice(g * HEAD, (g + 1) * HEAD)
            values = pool_ref[:, at_group].astype(f32)
            for n in range(4):
                sums[n, :lead, :] = jnp.zeros((lead, HEAD), f32)
            sums[0, lead : lead + reach, :] = rim_ref[:, at_group].astype(f32)
            sums[0, lead + reach :, :] = values
            steps = 3 if g == 0 else 4
            for n in range(1, steps):
                by = 2 ** (n - 1)
                sums[n, lead:, :] = sums[n - 1, lead:, :] + sums[n - 1, lead - by : end - by, :]
            start = lead + reach
            if g == 0:
                by = 4
                longer = sums[2, start:, :] + sums[2, start - by : end - by, :]
                shorter = sums[1, start:, :]
            else:
                by = 8
                longer = sums[3, start:, :] + sums[3, start - by : end - by, :]
                shorter = sums[2, start:, :]
            window = jnp.where(late, 8 if g == 0 else 16, 2 if g == 0 else 4)
            count = jnp.minimum(time, window).astype(f32)
            centred = (jnp.where(late, longer, shorter) / count - values).astype(bf16)
            mixed = jnp.dot(centred, map_ref[g], preferred_element_type=f32)
            scratch[:, at_group] = (mixed * gain_ref[:, at_group].astype(f32)).astype(bf16)
        to_destinations(at_ref, scratch, out_ref, own_rows)

    operands = (pool_in, rim, pool_map, gain)
    return pl.pallas_call(
        kernel,
        out_shape=jax.ShapeDtypeStruct((rows, cols), bf16),
        in_specs=[in_smem()] + [whole(a.shape) for a in operands],
        out_specs=whole((rows, cols)),
        scratch_shapes=[
            pltpu.VMEM((4, lead + reach + rows, HEAD), f32),
            pltpu.VMEM((rows, cols), bf16),
        ],
        compiler_params=params(16),
        name="pooling",
    )(at, *operands)


def leave(pool_mixed, mem_mixed, weights, first, count):
    rows, pool_cols = pool_mixed.shape
    mem_cols = mem_mixed.shape[1]
    width = weights.shape[2]
    half = rows // 2
    step = 2

    def kernel(pool_ref, mem_ref, weight_ref, own_ref, send_ref):
        for n in range(step):
            part = jnp.dot(pool_ref[...], weight_ref[n, :pool_cols], preferred_element_type=f32)
            part = part + jnp.dot(mem_ref[...], weight_ref[n, pool_cols:], preferred_element_type=f32)
            part = part.astype(bf16)
            own_ref[:, n * width : (n + 1) * width] = part[:half]
            send_ref[:, n * width : (n + 1) * width] = part[half:]

    shape = (half, width * count)
    out_spec = pl.BlockSpec((half, width * step), lambda i: (0, i))
    return pl.pallas_call(
        kernel,
        grid=(count // step,),
        out_shape=(jax.ShapeDtypeStruct(shape, bf16), jax.ShapeDtypeStruct(shape, bf16)),
        in_specs=[
            pl.BlockSpec((rows, pool_cols), lambda i: (0, 0)),
            pl.BlockSpec((rows, mem_cols), lambda i: (0, 0)),
            pl.BlockSpec((step, pool_cols + mem_cols, width), lambda i: (first // step + i, 0, 0)),
        ],
        out_specs=(out_spec, out_spec),
        compiler_params=params(16),
        name="leave",
    )(pool_mixed, mem_mixed, weights)


def scan_states(at, arrived, heads):
    devices, lines, width = arrived.shape
    share = (lines - 8) // heads

    def kernel(at_ref, arrived_ref, out_ref, peaks_ref):
        lane = lax.broadcasted_iota(jnp.int32, peaks_ref.shape, 1)
        peaks = jnp.zeros(peaks_ref.shape, f32)
        for h in range(heads):
            state = jnp.zeros((share, width), f32)
            peak, entering = jnp.zeros((1, 1), f32), jnp.zeros((1, 1), f32)
            for i in range(devices):
                entering = jnp.where(i == at_ref[2], peak, entering)
                out_ref[i, h] = state
                logs = arrived_ref[i, heads * share : heads * share + 1]
                decayed, fresh = logs[:, h : h + 1] + peak, logs[:, heads + h : heads + h + 1]
                joined = jnp.maximum(decayed, fresh)
                own = arrived_ref[i, h * share : (h + 1) * share]
                state = jnp.exp(decayed - joined) * state + jnp.exp(fresh - joined) * own
                peak = joined
            peaks = jnp.where(lane == h, entering, peaks)
        peaks_ref[...] = peaks

    shapes = [(devices, heads, share, width), (8, GATE_LANES)]
    return pl.pallas_call(
        kernel,
        out_shape=tuple(jax.ShapeDtypeStruct(s, f32) for s in shapes),
        in_specs=[in_smem(), whole(arrived.shape)],
        out_specs=tuple(whole(s) for s in shapes),
        compiler_params=params(8),
        name="scan_states",
    )(at, arrived)


def pair_up(own, came, own_rows):
    cols = own.shape[1]

    def kernel(own_ref, came_ref, here_ref, next_ref, last_ref, up_ref, down_ref):
        def total(k, part):
            rows = slice(k * own_rows, (k + 1) * own_rows)
            return (own_ref[rows, part].astype(f32) + came_ref[rows, part].astype(f32)).astype(bf16)

        every = slice(0, cols)
        up_ref[...] = total(2, slice(0, cols // 2))
        down_ref[...] = total(2, slice(cols // 2, cols))
        next_ref[...] = total(1, every)
        last_ref[...] = total(3, every)
        here_ref[...] = total(0, every)

    shapes = [(own_rows, cols)] * 3 + [(own_rows, cols // 2)] * 2
    return pl.pallas_call(
        kernel,
        out_shape=tuple(jax.ShapeDtypeStruct(s, bf16) for s in shapes),
        in_specs=[whole(own.shape)] * 2,
        out_specs=tuple(whole(s) for s in shapes),
        compiler_params=params(8),
        name="pair_up",
    )(own, came)


def relay(following, last, up, down):
    rows, cols = following.shape
    middle = cols // 2

    def kernel(next_ref, last_ref, up_ref, down_ref, to_next, to_last):
        to_next[:, :middle] = (next_ref[:, :middle].astype(f32) + up_ref[...].astype(f32)).astype(bf16)
        to_next[:, middle:] = next_ref[:, middle:]
        to_last[:, :middle] = last_ref[:, :middle]
        to_last[:, middle:] = (last_ref[:, middle:].astype(f32) + down_ref[...].astype(f32)).astype(bf16)

    return pl.pallas_call(
        kernel,
        out_shape=tuple(jax.ShapeDtypeStruct((rows, cols), bf16) for _ in range(2)),
        in_specs=[whole(a.shape) for a in (following, last, up, down)],
        out_specs=tuple(whole((rows, cols)) for _ in range(2)),
        compiler_params=params(8),
        name="relay",
    )(following, last, up, down)


def finish(groups):
    rows, cols = groups[0][0].shape
    flat = [a for group in groups for a in group]
    count = len(groups[0])

    def kernel(*refs):
        out_ref = refs[-1]
        for g in range(len(groups)):
            total = None
            for ref in refs[g * count : (g + 1) * count]:
                part = ref[...].astype(f32)
                total = part if total is None else total + part
            out_ref[:, g * cols : (g + 1) * cols] = total.astype(bf16)

    shape = (rows, cols * len(groups))
    return pl.pallas_call(
        kernel,
        out_shape=jax.ShapeDtypeStruct(shape, bf16),
        in_specs=[whole((rows, cols))] * len(flat),
        out_specs=whole(shape),
        compiler_params=params(8),
        name="finish",
    )(*flat)


def on_device(
    tokens,
    norm_gain,
    w_pool_in,
    w_mem_in,
    w_input_gate,
    w_forget_gate,
    forget_bias,
    forget_extra,
    conv_weight,
    query_map,
    key_map,
    pool_map,
    pool_gain,
    mem_gain,
    w_out_pool,
    w_out_mem,
):
    x_index = lax.axis_index("x")
    core_index = lax.axis_index("core")
    tp_index = lax.axis_index(TP)
    sp_index = lax.axis_index(SP)
    sp_size = lax.axis_size(SP)
    chips = lax.axis_size("x")
    own_rows = tokens.shape[0]
    seq_rows = own_rows * lax.axis_size(TP)
    group_count = pool_map.shape[0]
    pool_cols = group_count * HEAD
    head_count = forget_extra.shape[1]
    mem_cols = head_count * HEAD
    blocks = seq_rows // BLOCK

    at = jnp.stack([lax.axis_index("z"), lax.axis_index("y"), sp_index, x_index, core_index, tp_index])
    pool_at, mem_at = tp_index * pool_cols, tp_index * mem_cols

    w_out = lax.all_gather(
        jnp.concatenate([w_out_pool, w_out_mem], axis=0), SP, axis=0, tiled=False
    )

    w_in = jnp.concatenate([w_mem_in, w_pool_in], axis=1)
    rings = [("y", "z"), ("z", "y")]
    phase = [
        first_phase(w_in[n * HALF_ROWS : (n + 1) * HALF_ROWS], rings[n][0]) for n in range(2)
    ]
    cut = w_mem_in.shape[1]
    w_mem = [second_phase(*(a[..., :cut] for a in phase[n]), rings[n][1]) for n in range(2)]
    w_pool = [second_phase(*(a[..., cut:] for a in phase[n]), rings[n][1]) for n in range(2)]

    normalized = norm_rows(at, tokens, norm_gain.reshape(1, D), w_input_gate, w_forget_gate)
    pieces = [normalized] + [shifted(normalized, "x", k) for k in range(1, chips)]
    core_pieces = [shifted(piece, "core", 1) for piece in pieces]
    rows_all, col, row, logs = assemble(at, forget_bias, forget_extra, pieces, core_pieces)

    def dense_map(map_table):
        own_blocks = lax.dynamic_slice_in_dim(map_table, mem_at // 4, mem_cols // 4, 0)
        own_blocks = own_blocks.reshape(mem_cols, 4)
        place = (jnp.arange(HEAD)[None, :] % 4 == jnp.arange(4)[:, None]).astype(bf16)
        spread = jnp.dot(own_blocks, place, preferred_element_type=f32)
        same = (jnp.arange(mem_cols)[:, None] % HEAD) // 4 == jnp.arange(HEAD)[None, :] // 4
        return jnp.where(same, spread, 0.0).astype(bf16).reshape(head_count, HEAD, HEAD)

    conv_own = lax.dynamic_slice_in_dim(conv_weight, mem_at, mem_cols, 1)
    mem_in, mem_rim = enter(rows_all, *w_mem, 8, "enter_mem")
    mem_rim = passed_along(mem_rim, SP, 1)
    hidden, query, weight, own_state = memory_before(
        sp_size, logs, mem_in, mem_rim, conv_own, dense_map(query_map), dense_map(key_map), col, row
    )
    arrived = lax.all_to_all(own_state, SP, split_axis=0, concat_axis=0, tiled=True)
    starts, peaks = scan_states(at, arrived, head_count)
    states = lax.all_to_all(starts, SP, split_axis=0, concat_axis=0, tiled=True)
    mem_gain_own = lax.dynamic_slice_in_dim(mem_gain, mem_at, mem_cols, 0).reshape(1, mem_cols)
    mem_mixed = memory_after(
        at, hidden, query, weight, states, peaks, mem_gain_own, own_rows
    )

    pool_in, pool_rim = enter(rows_all, *w_pool, 16, "enter_pool")
    pool_rim = passed_along(pool_rim, SP, 1)
    pool_gain_own = lax.dynamic_slice_in_dim(pool_gain, pool_at, pool_cols, 0).reshape(1, pool_cols)
    pool_mixed = pooling(at, pool_in, pool_rim, pool_map, pool_gain_own, own_rows)

    groups = []
    for n in range(OUT_CHUNKS):
        count = sp_size // OUT_CHUNKS
        own, send = leave(pool_mixed, mem_mixed, w_out, n * count, count)
        here, following, last, up, down = pair_up(own, shifted(send, "core", 1), own_rows)
        up, down = shifted(up, "x", 1), shifted(down, "x", -1)
        following, last = relay(following, last, up, down)
        groups.append([here, shifted(following, "x", 1), shifted(last, "x", -1)])
    return finish(groups)


def solution(mesh):
    torus = Mesh(mesh.devices.reshape(4, 4, mesh.shape["tp"] // 2, 2), ("z", "y", "x", "core"))
    in_specs = (
        P(SP_TP, None),
        P(),
        P(SP, TP),
        P(SP, TP),
        P(),
        P(),
        P(),
        P(SP, TP),
        P(),
        P(),
        P(),
        P(TP, None, None),
        P(),
        P(),
        P(TP, SP),
        P(TP, SP),
    )
    out_specs = P(SP_TP, None)
    return jax.shard_map(
        on_device, mesh=torus, in_specs=in_specs, out_specs=out_specs, check_vma=False
    )
```
